32 devices in a mesh: rep: 2 (over x), fs: 8 (over z, y), tp: 2 (over core).
Axes of the slice: x: 2, y: 2, z: 4, core: 2. Of those that a mesh axis runs over, the one named last changes fastest.
Arguments:
- tokens: bfloat16 [16, 256, 1024], P(('rep', 'fs'), None, 'tp'), may hold values from -6 to 6
- pre_gain: float32 [1024], replicated, may hold values from 0.1 to 1.9
- first_gate: bfloat16 [1024, 2560], P('fs', 'tp'), may hold values from -0.1875 to 0.1875
- first_up: bfloat16 [1024, 2560], P('fs', 'tp'), may hold values from -0.1875 to 0.1875
- first_down: bfloat16 [2560, 1024], P('tp', 'fs'), may hold values from -0.125 to 0.125
- mix_gain: float32 [1024], P('tp'), may hold values from 0.1 to 1.9
- pool_weight: bfloat16 [4, 256, 256], P('tp', None, 'fs'), may hold values from -0.375 to 0.375
- pool_scale: float32 [1024], P('tp'), may hold values from 0.1 to 1.9
- post_gain: float32 [1024], replicated, may hold values from 0.1 to 1.9
- second_gate: bfloat16 [1024, 2560], P('fs', 'tp'), may hold values from -0.1875 to 0.1875
- second_up: bfloat16 [1024, 2560], P('fs', 'tp'), may hold values from -0.1875 to 0.1875
- second_down: bfloat16 [2560, 1024], P('tp', 'fs'), may hold values from -0.125 to 0.125
Outputs:
- layer_out: bfloat16 [16, 256, 1024], P(('rep', 'fs'), None, 'tp')
The draws below stay inside these ranges and needn't reach their ends.
All inputs are finite; a program needn't handle non-finite values.
Results may differ from the reference program's by a relative error of at most 0.015.
Values may be sent and summed in bfloat16 or wider, within the bound.
A program may use at most 64 MiB of HBM per device.

```python
import jax
import jax.numpy as jnp
from jax import lax

D = 1024
FF = 2560
GROUPS = 4
GROUP = 256
SEQ = 256
BATCH = 16


def levels(stream_key, extent, cuts, least, high):
    loudness = 1.0
    for axis_at, shards_of in cuts:
        steps = jax.random.uniform(jax.random.fold_in(jax.random.fold_in(stream_key, 6), axis_at), (shards_of,), jnp.float32, least / len(cuts), high / len(cuts))
        loudness = loudness * jnp.repeat(jnp.exp(steps), extent[axis_at] // shards_of).reshape((-1,) + (1,) * (len(extent) - 1 - axis_at))
    return loudness


def scatter_about(own_key, shape, deviation, reach, shards=(), held_as=jnp.bfloat16):
    values = deviation * jax.random.normal(own_key, shape, jnp.float32)
    if shards:
        values = values * levels(own_key, shape, shards, -0.22, 0.18)
    return jnp.clip(values, -reach, reach).astype(held_as)


def setup_inputs(seed: int = 0) -> dict:
    key_of = jax.random.split(jax.random.key(seed), 13)
    tokens = scatter_about(key_of[0], (BATCH, SEQ, D), 1.0, 6.0, ((0, 16), (2, 2)))
    pre_gain = jnp.clip(1.0 + 0.18 * jax.random.normal(key_of[1], (D,), jnp.float32), 0.1, 1.9)
    first_gate = scatter_about(key_of[2], (D, FF), D ** -0.5, 0.1875, ((0, 8), (1, 2)))
    first_up = scatter_about(key_of[3], (D, FF), D ** -0.5, 0.1875, ((0, 8), (1, 2)))
    first_down = scatter_about(key_of[4], (FF, D), FF ** -0.5, 0.125, ((0, 2), (1, 8)))
    mix_gain = jnp.clip(1.0 + 0.18 * jax.random.normal(key_of[5], (D,), jnp.float32), 0.1, 1.9)
    pool_weight = scatter_about(key_of[6], (GROUPS, GROUP, GROUP), GROUP ** -0.5, 0.375, ((0, 2), (2, 8)))
    pool_scale = jnp.clip(1.0 + 0.18 * jax.random.normal(key_of[7], (D,), jnp.float32), 0.1, 1.9)
    post_gain = jnp.clip(1.0 + 0.18 * jax.random.normal(key_of[8], (D,), jnp.float32), 0.1, 1.9)
    second_gate = scatter_about(key_of[9], (D, FF), D ** -0.5, 0.1875, ((0, 8), (1, 2)))
    second_up = scatter_about(key_of[10], (D, FF), D ** -0.5, 0.1875, ((0, 8), (1, 2)))
    second_down = scatter_about(key_of[11], (FF, D), FF ** -0.5, 0.125, ((0, 2), (1, 8)))
    return dict(tokens=tokens, pre_gain=pre_gain, first_gate=first_gate, first_up=first_up, first_down=first_down, mix_gain=mix_gain, pool_weight=pool_weight, pool_scale=pool_scale, post_gain=post_gain, second_gate=second_gate, second_up=second_up, second_down=second_down)


epsilon = 1e-06

def normalize(values, gain_vec):
    floats = values.astype(jnp.float32)
    scaled = floats * lax.rsqrt(lax.optimization_barrier(jnp.mean(floats * floats, axis=-1, keepdims=True)) + epsilon)
    return (scaled * gain_vec.astype(jnp.float32)).astype(jnp.bfloat16)

def half_block(flat_rows, gain_vec, gate_w, up_w, down_w):
    normed = normalize(flat_rows, gain_vec)
    gate_sum = jnp.dot(normed, gate_w, preferred_element_type=jnp.float32)
    up_sum = jnp.dot(normed, up_w, preferred_element_type=jnp.float32)
    hidden = (jax.nn.silu(gate_sum) * up_sum).astype(jnp.bfloat16)
    return jnp.dot(hidden, down_w, preferred_element_type=jnp.float32)

def trailing(grouped, windows, widest):
    seq_length = grouped.shape[1]
    running = jnp.zeros_like(grouped)
    for back_step in range(widest):
        moved = jnp.pad(grouped, ((0, 0), (back_step, 0), (0, 0), (0, 0)))[:, :seq_length]
        running = running + jnp.where(back_step < windows[None, None, :, None], moved, 0.0)
    positions = jnp.arange(seq_length, dtype=jnp.int32)
    counts = jnp.minimum(positions[:, None] + 1, windows[None, :]).astype(jnp.float32)
    return running / counts[None, :, :, None]

def reference(tokens, pre_gain, first_gate, first_up, first_down, mix_gain, pool_weight, pool_scale, post_gain, second_gate, second_up, second_down):
    flat_rows = tokens.reshape(BATCH * SEQ, D)
    first_out = half_block(flat_rows, pre_gain, first_gate, first_up, first_down)
    after_first = (flat_rows.astype(jnp.float32) + 0.5 * first_out).astype(jnp.bfloat16)
    normed = normalize(after_first, mix_gain)
    grouped = normed.astype(jnp.float32).reshape(BATCH, SEQ, GROUPS, GROUP)
    windows = 2 ** (jnp.arange(GROUPS, dtype=jnp.int32) + 1)
    pooled = trailing(grouped, windows, 2 ** GROUPS)
    diff = (pooled - grouped).astype(jnp.bfloat16)
    mixed = jnp.einsum('bsgc,gcd->bsgd', diff.astype(jnp.float32), pool_weight.astype(jnp.float32))
    mixed = mixed.reshape(BATCH * SEQ, D)
    after_mix = (after_first.astype(jnp.float32) + mixed * pool_scale.astype(jnp.float32)).astype(jnp.bfloat16)
    second_out = half_block(after_mix, post_gain, second_gate, second_up, second_down)
    layer_out = (after_mix.astype(jnp.float32) + 0.5 * second_out).astype(jnp.bfloat16)
    return layer_out.reshape(BATCH, SEQ, D)
```

```python
import functools

import jax
import jax.numpy as jnp
from jax import lax
from jax.experimental import pallas as pl
from jax.experimental.pallas import tpu as pltpu
from jax.sharding import PartitionSpec as P

D = 1024
GROUPS = 4


epsilon = 1e-06


def taken_in(shard, axis, dim, take_in, carry):
    whole = jax.tree.map(lambda part: lax.all_gather(part, axis, axis=dim, tiled=True), shard)
    return take_in(carry, whole, jnp.int32(0))


def over_all(shard, axis, dim, block):
    whole = lax.all_gather(shard, axis, axis=dim, tiled=True)
    return block(whole, jnp.int32(0))


def normalize(values, gain_vec):
    floats = values.astype(jnp.float32)
    scaled = floats * lax.rsqrt(jnp.mean(floats * floats, axis=-1, keepdims=True) + epsilon)
    return (scaled * gain_vec.astype(jnp.float32)).astype(jnp.bfloat16)


def half_step(local_part, gain_vec, gate_w, up_w, down_w):
    gathered = lax.all_gather(local_part, "tp", axis=2, tiled=True)
    seq_count, seq_length, full_width = gathered.shape
    normed = normalize(gathered.reshape(seq_count * seq_length, full_width), gain_vec)
    zero_init = jnp.zeros((normed.shape[0], gate_w.shape[1]), jnp.float32)

    def add_rows(running, block_rows, offset):
        columns = lax.dynamic_slice_in_dim(normed, offset, block_rows.shape[0], 1)
        return running + jnp.dot(columns, block_rows, preferred_element_type=jnp.float32)

    gate_sum = taken_in(gate_w, "fs", 0, add_rows, zero_init)
    up_sum = taken_in(up_w, "fs", 0, add_rows, zero_init)
    hidden = (jax.nn.silu(gate_sum) * up_sum).astype(jnp.bfloat16)

    def project(block_cols, offset):
        return jnp.dot(hidden, block_cols, preferred_element_type=jnp.float32)

    partial_value = over_all(down_w, "fs", 1, project)
    own_part = lax.psum_scatter(
        partial_value.astype(jnp.bfloat16), "tp", scatter_dimension=1, tiled=True
    ).astype(jnp.float32)
    return own_part.reshape(seq_count, seq_length, own_part.shape[1])


def trailing(grouped, windows, widest):
    seq_length = grouped.shape[1]
    running = jnp.zeros_like(grouped)
    for back_step in range(widest):
        moved = jnp.pad(grouped, ((0, 0), (back_step, 0), (0, 0), (0, 0)))[:, :seq_length]
        running = running + jnp.where(back_step < windows[None, None, :, None], moved, 0.0)
    positions = jnp.arange(seq_length, dtype=jnp.int32)
    counts = jnp.minimum(positions[:, None] + 1, windows[None, :]).astype(jnp.float32)
    return running / counts[None, :, :, None]


def pool_mix(local_part, mix_gain, pool_weight, pool_scale):
    floats = local_part.astype(jnp.float32)
    squares = lax.psum(jnp.sum(floats * floats, axis=-1).astype(jnp.bfloat16), "tp").astype(
        jnp.float32
    )
    normed = (
        floats * lax.rsqrt(squares[..., None] / D + epsilon) * mix_gain.astype(jnp.float32)
    ).astype(jnp.bfloat16)
    seq_count, seq_length, part_width = local_part.shape
    groups_here = pool_weight.shape[0]
    group_width = pool_weight.shape[1]
    grouped = normed.astype(jnp.float32).reshape(seq_count, seq_length, groups_here, group_width)
    group_ids = lax.axis_index("tp") * groups_here + jnp.arange(groups_here, dtype=jnp.int32)
    windows = 2 ** (group_ids + 1)
    pooled = trailing(grouped, windows, 2**GROUPS)
    diff = (pooled - grouped).astype(jnp.bfloat16)

    def mix_cols(block_cols, offset):
        return jnp.einsum("bsgc,gcd->bsgd", diff, block_cols, preferred_element_type=jnp.float32)

    mixed = over_all(pool_weight, "fs", 2, mix_cols)
    mixed = mixed.reshape(seq_count, seq_length, part_width)
    return (floats + mixed * pool_scale.astype(jnp.float32)).astype(jnp.bfloat16)


def local(
    tokens,
    pre_gain,
    first_gate,
    first_up,
    first_down,
    mix_gain,
    pool_weight,
    pool_scale,
    post_gain,
    second_gate,
    second_up,
    second_down,
):
    first_out = half_step(tokens, pre_gain, first_gate, first_up, first_down)
    after_first = (tokens.astype(jnp.float32) + 0.5 * first_out).astype(jnp.bfloat16)
    after_mix = pool_mix(after_first, mix_gain, pool_weight, pool_scale)
    second_out = half_step(after_mix, post_gain, second_gate, second_up, second_down)
    return (after_mix.astype(jnp.float32) + 0.5 * second_out).astype(jnp.bfloat16)


F32 = jnp.float32
BF16 = jnp.bfloat16


def layer_kernel(
    nz, tok_ref, pre_ref, mixg_ref, scale_ref, post_ref, pw_ref, tail1_ref, tail2_ref,
    g1_ref, u1_ref, d1_ref, g2_ref, u2_ref, d2_ref, out_ref,
    GU, DW, PW, T, N, ACC, H, PS, PR, S, R, SQ,
    sw_s, sw_r, loc, zs, zr, ts, tr, cs, cr, os_, or_, ps_, pr_, qs, qr,
):
    r = lax.axis_index("rep")
    f = lax.axis_index("fs")
    t = lax.axis_index("tp")
    x = lax.rem(r, 2)
    y = lax.rem(f, 2)
    z = f // 2
    rx = r + 1 - 2 * x
    fy = f + 1 - 2 * y
    me = 2 * x + y
    other = 1 - t

    def dev(rr, ff, tt):
        return {"rep": rr, "fs": ff, "tp": tt}

    quad = (dev(rx, f, t), dev(r, fy, t), dev(rx, fy, t))
    quad_idx = (2 * (1 - x) + y, 2 * x + (1 - y), 2 * (1 - x) + (1 - y))
    mate = dev(r, f, other)
    above = dev(r, f + 2, t)
    below = dev(r, f - 2, t)
    has_above = z < nz - 1
    has_below = z > 0

    barrier = pltpu.get_barrier_semaphore()
    for peer in quad + (mate,):
        pl.semaphore_signal(barrier, inc=1, device_id=peer, device_id_type=pl.DeviceIdType.MESH)

    @pl.when(has_above)
    def _():
        pl.semaphore_signal(barrier, inc=1, device_id=above, device_id_type=pl.DeviceIdType.MESH)

    @pl.when(has_below)
    def _():
        pl.semaphore_signal(barrier, inc=1, device_id=below, device_id_type=pl.DeviceIdType.MESH)

    def remote(src, dst, ss, rs, to):
        return pltpu.make_async_remote_copy(
            src_ref=src, dst_ref=dst, send_sem=ss, recv_sem=rs,
            device_id=to, device_id_type=pl.DeviceIdType.MESH,
        )

    rows, half = tok_ref.shape
    depth = g1_ref.shape[0]
    main = (g1_ref.shape[1] // 512) * 128
    rest = g1_ref.shape[1] // 4 - main
    big = GU.shape[-1]
    cw = d1_ref.shape[1]
    weights = ((g1_ref, u1_ref, tail1_ref, d1_ref), (g2_ref, u2_ref, tail2_ref, d2_ref))

    def pieces(b, q):
        g, u, tl, d = weights[b]
        lanes = pl.ds(pl.multiple_of(q * main, 128), main)
        ends = pl.ds(pl.multiple_of(q * 2 * rest, 128), 2 * rest)
        deep = pl.ds(pl.multiple_of(y * depth, 128), depth)
        rows_main = pl.ds(pl.multiple_of(q * main, 128), main)
        rows_rest = pl.ds(pl.multiple_of(4 * main + q * rest, 16), rest)
        return (
            (g.at[:, lanes], GU.at[b, z, deep, 0:main]),
            (u.at[:, lanes], GU.at[b, z, deep, main:2 * main]),
            (tl.at[:, ends], GU.at[b, z, deep, 2 * main:big]),
            (d.at[rows_main, :], DW.at[b, z, y, 0:main, :]),
            (d.at[rows_rest, :], DW.at[b, z, y, main:main + rest, :]),
        )

    def own_copies(b):
        found = [pltpu.make_async_copy(s, d, loc.at[b, i]) for i, (s, d) in enumerate(pieces(b, me))]
        if b == 0:
            found.append(pltpu.make_async_copy(pw_ref, PW.at[z, y], loc.at[b, 5]))
        return found

    def swaps(b):
        found = [
            remote(s, d, sw_s.at[b, i], sw_r.at[b, i], quad[1])
            for i, (s, d) in enumerate(pieces(b, quad_idx[1]))
        ]
        if b == 0:
            found.append(remote(pw_ref, PW.at[z, y], sw_s.at[b, 5], sw_r.at[b, 5], quad[1]))
        return found

    kinds = (GU, DW)

    def z_up(b, k, kind):
        p = jnp.maximum(z - k, 0)
        ref = PW.at[p] if kind == 2 else kinds[kind].at[b, p]
        return remote(ref, ref, zs.at[0, b, k, kind], zr.at[0, b, k, kind], above)

    def z_down(b, k, kind):
        p = jnp.minimum(z + k, nz - 1)
        ref = PW.at[p] if kind == 2 else kinds[kind].at[b, p]
        return remote(ref, ref, zs.at[1, b, k, kind], zr.at[1, b, k, kind], below)

    def can_up(k):
        return jnp.logical_and(has_above, z - k >= 0)

    def can_down(k):
        return jnp.logical_and(has_below, z + k <= nz - 1)

    def z_send(b, k, kind):
        @pl.when(can_up(k))
        def _():
            z_up(b, k, kind).start()

        @pl.when(can_down(k))
        def _():
            z_down(b, k, kind).start()

    def z_sent(b, k, kind):
        @pl.when(can_up(k))
        def _():
            z_up(b, k, kind).wait_send()

        @pl.when(can_down(k))
        def _():
            z_down(b, k, kind).wait_send()

    def z_take(b, k, kind):
        @pl.when(z - 1 - k >= 0)
        def _():
            z_up(b, k, kind).wait_recv()

        @pl.when(z + 1 + k <= nz - 1)
        def _():
            z_down(b, k, kind).wait_recv()

        if k + 1 < nz - 1:
            z_send(b, k + 1, kind)

    def tok_sends(b):
        mine = T.at[b, me, t]
        return [remote(mine, mine, ts.at[b, j], tr.at[b, j], quad[j]) for j in range(3)]

    def mate_own(b):
        mine = T.at[b, me, t]
        return remote(mine, mine, os_.at[b], or_.at[b], mate)

    def mate_pass(b, j):
        got = T.at[b, quad_idx[j], t]
        return remote(got, got, cs.at[b, j], cr.at[b, j], mate)

    def order(i):
        m = jnp.minimum(z, nz - 1 - z)
        near = z - (i + 1) // 2 if i % 2 else z + i // 2
        far = jnp.where(2 * z < nz - 1, i, nz - 1 - i)
        return jnp.where(i <= 2 * m, near, far)

    def norm_block(b, q, gain_ref):
        parts = [T[b, q, c].astype(F32) for c in range(2)]
        total = sum(jnp.sum(v * v, axis=-1, keepdims=True) for v in parts)
        inv = lax.rsqrt(total / (2 * half) + epsilon)
        step = N.shape[2]
        for c in range(2):
            done = (parts[c] * inv * gain_ref[0:1, c * half:(c + 1) * half]).astype(BF16)
            for i in range(half // step):
                N[c * (half // step) + i, pl.ds(pl.multiple_of(q * rows, 128), rows), :] = done[:, i * step:(i + 1) * step]

    def gate_up(b, i):
        p = order(i)

        @pl.loop(0, 4)
        def _(q):
            at = pl.ds(pl.multiple_of(q * rows, 128), rows)
            value = jnp.dot(N[p, at, :], GU[b, p], preferred_element_type=F32)
            if i == 0:
                ACC[at, :] = value
            else:
                ACC[at, :] += value

    def hidden_of():
        @pl.loop(0, 4)
        def _(q):
            at = pl.ds(pl.multiple_of(q * rows, 128), rows)
            gate = ACC[at, 0:main]
            up = ACC[at, main:2 * main]
            H[at, 0:main] = (jax.nn.silu(gate) * up).astype(BF16)
            last = ACC[at, 2 * main:big]
            H[at, main:main + rest] = (jax.nn.silu(last[:, :rest]) * last[:, rest:]).astype(BF16)

    def half_sends(b):
        span = pl.ds(other * (nz // 2), nz // 2)
        return [
            remote(
                PS.at[b, q, span], PR.at[b, q], ps_.at[b, q], pr_.at[b, q], mate
            )
            for q in range(4)
        ]

    def down(b):
        sends = half_sends(b)
        for q in range(4):
            for p in range(nz):
                wide = jnp.concatenate([DW[b, p, 0], DW[b, p, 1]], axis=1)
                PS[b, q, p] = jnp.dot(
                    H[q * rows:(q + 1) * rows, :], wide, preferred_element_type=F32
                ).astype(BF16)
            sends[q].start()

    def sum_half(b, q):
        for i in range(nz // 2):
            mine = PS[b, q, t * (nz // 2) + i].astype(F32)
            S[b, q, :, i * 2 * cw:(i + 1) * 2 * cw] = (mine + PR[b, q, i].astype(F32)).astype(BF16)

    def quad_sends(b):
        return [
            remote(S.at[b, quad_idx[j]], R.at[b, j], qs.at[b, j], qr.at[b, j], quad[j])
            for j in range(3)
        ]

    def scatter(b):
        sends = half_sends(b)
        for q in range(4):
            sends[q].wait_recv()
            sum_half(b, q)
        for j in (2, 1, 0):
            quad_sends(b)[j].start()

    def collect(b):
        for send in quad_sends(b):
            send.wait_recv()
        total = S[b, me].astype(F32)
        for j in range(3):
            total = total + R[b, j].astype(F32)
        return total

    for c in own_copies(0):
        c.start()
    T[0, me, t] = tok_ref[...]
    pl.semaphore_wait(
        barrier, 4 + jnp.minimum(z, 1) + jnp.minimum(nz - 1 - z, 1)
    )

    for c in swaps(0)[:5]:
        c.start()
    for j in (0, 2, 1):
        tok_sends(0)[j].start()
    mate_own(0).start()
    swaps(0)[5].start()
    for c in own_copies(1):
        c.start()
    for c in swaps(1):
        c.start()
    for i, c in enumerate(own_copies(0)):
        c.wait()
    for i in (0, 1, 2):
        swaps(0)[i].wait_recv()
    z_send(0, 0, 0)
    for i in (3, 4):
        swaps(0)[i].wait_recv()
    z_send(0, 0, 1)
    mate_own(0).wait_recv()
    norm_block(0, me, pre_ref)
    for j in (0, 2, 1):
        tok_sends(0)[j].wait_recv()
        mate_pass(0, j).start()
    for j in (0, 2, 1):
        mate_pass(0, j).wait_recv()
        norm_block(0, quad_idx[j], pre_ref)
    swaps(0)[5].wait_recv()
    gate_up(0, 0)
    for k in range(nz - 1):
        z_take(0, k, 0)
        gate_up(0, k + 1)
        z_take(0, k, 1)
        if k == 0:
            z_send(0, 0, 2)
        else:
            z_take(0, k - 1, 2)
        if k == max(nz - 3, 0):
            for c in own_copies(1):
                c.wait()
            for c in swaps(1):
                c.wait_recv()
            z_send(1, 0, 0)
            z_send(1, 0, 1)
    hidden_of()
    down(0)
    scatter(0)
    z_take(0, nz - 2, 2)
    z_take(1, 0, 0)
    z_take(1, 0, 1)
    first = collect(0)
    after_first = (tok_ref[...].astype(F32) + 0.5 * first).astype(BF16).astype(F32)
    square = after_first * after_first
    SQ[0] = sum(square[:, i * 128:(i + 1) * 128] for i in range(half // 128))
    swap_sq = remote(SQ.at[0], SQ.at[1], os_.at[2], or_.at[2], mate)
    swap_sq.start()
    swap_sq.wait_recv()
    total = jnp.sum(SQ[0] + SQ[1], axis=-1, keepdims=True)
    h = (after_first * lax.rsqrt(total / (2 * half) + epsilon) * mixg_ref[0:1, :]).astype(BF16).astype(F32)
    position = lax.broadcasted_iota(jnp.int32, (rows, 128), 0)
    groups_here = pw_ref.shape[0]
    width = half // groups_here

    def shifted(v, by):
        place = lax.broadcasted_iota(jnp.int32, v.shape, 0)
        return jnp.where(place >= by, pltpu.roll(v, by, 0), 0.0)

    for g in range(groups_here):
        hg = h[:, g * width:(g + 1) * width]
        run = hg + shifted(hg, 1)
        window = 2
        found = run
        number = t * groups_here + g
        reached = jnp.int32(2)
        for level in range(1, GROUPS):
            run = run + shifted(run, window)
            window = window * 2
            found = jnp.where(number >= level, run, found)
            reached = jnp.where(number >= level, window, reached)
        counts = jnp.minimum(lax.broadcasted_iota(jnp.int32, (rows, width), 0) + 1, reached).astype(F32)
        diff = (found / counts - hg).astype(BF16)
        turned = jnp.concatenate([PW[i // 2, i % 2, g] for i in range(2 * nz)], axis=0)
        mixed = lax.dot_general(diff, turned, (((1,), (1,)), ((), ())), preferred_element_type=F32)
        at = slice(g * width, (g + 1) * width)
        T[1, me, t, :, at] = (after_first[:, at] + scale_ref[0:1, at] * mixed).astype(BF16)
    for j in (0, 2, 1):
        tok_sends(1)[j].start()
    mate_own(1).start()
    z_take(1, 1, 0)
    z_take(1, 1, 1)
    mate_own(1).wait_recv()
    norm_block(1, me, post_ref)
    for j in (0, 2, 1):
        tok_sends(1)[j].wait_recv()
        mate_pass(1, j).start()
    for j in (0, 2, 1):
        mate_pass(1, j).wait_recv()
        norm_block(1, quad_idx[j], post_ref)
    for i in range(nz - 1):
        gate_up(1, i)
    for k in range(2, nz - 1):
        z_take(1, k, 0)
        z_take(1, k, 1)
    gate_up(1, nz - 1)
    hidden_of()
    down(1)
    scatter(1)
    out_ref[...] = (T[1, me, t].astype(F32) + 0.5 * collect(1)).astype(BF16)

    for b in range(2):
        for c in swaps(b) + tok_sends(b) + [mate_own(b)] + [mate_pass(b, j) for j in range(3)]:
            c.wait_send()
        for c in half_sends(b) + quad_sends(b):
            c.wait_send()
        for k in range(nz - 1):
            for kind in range(3 if b == 0 else 2):
                z_sent(b, k, kind)
    swap_sq.wait_send()


def fused(
    fs, tokens, pre_gain, first_gate, first_up, first_down, mix_gain, pool_weight,
    pool_scale, post_gain, second_gate, second_up, second_down,
):
    nz = fs // 2
    _, rows, half = tokens.shape
    depth, hid = first_gate.shape
    cw = first_down.shape[1]
    main = (hid // 512) * 128
    rest = hid // 4 - main
    groups, width, out_cols = pool_weight.shape

    def tail_of(gate, up):
        parts = [v[:, 4 * main:].reshape(depth, 4, rest) for v in (gate, up)]
        return jnp.concatenate(parts, axis=2).reshape(depth, 8 * rest)

    vmem = pl.BlockSpec(memory_space=pltpu.VMEM)
    anyw = pl.BlockSpec(memory_space=pl.ANY)
    dma = pltpu.SemaphoreType.DMA
    big = 2 * main + 2 * rest
    steps = nz - 1
    out = pl.pallas_call(
        functools.partial(layer_kernel, nz),
        out_shape=jax.ShapeDtypeStruct((rows, half), BF16),
        in_specs=[vmem] * 6 + [anyw] * 8,
        out_specs=vmem,
        scratch_shapes=[
            pltpu.VMEM((2, nz, 2 * depth, big), BF16),
            pltpu.VMEM((2, nz, 2, main + rest, cw), BF16),
            pltpu.VMEM((nz, 2, groups, out_cols, width), BF16),
            pltpu.VMEM((2, 4, 2, rows, half), BF16),
            pltpu.VMEM((nz, 4 * rows, 2 * depth), BF16),
            pltpu.VMEM((4 * rows, big), F32),
            pltpu.VMEM((4 * rows, main + rest), BF16),
            pltpu.VMEM((2, 4, nz, rows, 2 * cw), BF16),
            pltpu.VMEM((2, 4, nz // 2, rows, 2 * cw), BF16),
            pltpu.VMEM((2, 4, rows, half), BF16),
            pltpu.VMEM((2, 3, rows, half), BF16),
            pltpu.VMEM((2, rows, 128), F32),
            dma((2, 6)), dma((2, 6)), dma((2, 6)),
            dma((2, 2, steps, 3)), dma((2, 2, steps, 3)),
            dma((2, 3)), dma((2, 3)), dma((2, 3)), dma((2, 3)),
            dma((3,)), dma((3,)), dma((2, 4)), dma((2, 4)), dma((2, 3)), dma((2, 3)),
        ],
        compiler_params=pltpu.CompilerParams(
            collective_id=0, has_side_effects=True, vmem_limit_bytes=60 * 1024 * 1024
        ),
    )(
        tokens.reshape(rows, half), pre_gain.reshape(1, -1), mix_gain.reshape(1, -1),
        pool_scale.reshape(1, -1), post_gain.reshape(1, -1), jnp.swapaxes(pool_weight, 1, 2),
        tail_of(first_gate, first_up), tail_of(second_gate, second_up),
        first_gate, first_up, first_down, second_gate, second_up, second_down,
    )
    return out.reshape(tokens.shape)


def whole_tiles(mesh, args):
    reps, fs, tp = (mesh.shape[name] for name in ("rep", "fs", "tp"))
    depth = args[2].shape[0] // fs
    hid = args[2].shape[1] // tp
    return (
        tp == 2 and reps % 2 == 0 and fs % 8 == 0 and depth % 128 == 0
        and args[0].shape[0] == reps * fs and args[4].shape[1] // fs == depth
        and hid % 512 == 256 and args[6].shape[2] % (fs * 16) == 0
    )


def solution(mesh):
    placed = (
        P(("rep", "fs"), None, "tp"),
        P(),
        P("fs", "tp"),
        P("fs", "tp"),
        P("tp", "fs"),
        P("tp"),
        P("tp", None, "fs"),
        P("tp"),
        P(),
        P("fs", "tp"),
        P("fs", "tp"),
        P("tp", "fs"),
    )
    def layer(*args):
        body = functools.partial(fused, mesh.shape["fs"]) if whole_tiles(mesh, args) else local
        return jax.shard_map(
            body, mesh=mesh, in_specs=placed, out_specs=P(("rep", "fs"), None, "tp"), check_vma=False
        )(*args)

    return layer
```

```python
import functools

import jax
import jax.numpy as jnp
from jax import lax
from jax.experimental import pallas as pl
from jax.experimental.pallas import tpu as pltpu
from jax.sharding import PartitionSpec as P

D = 1024
GROUPS = 4


epsilon = 1e-06


def taken_in(shard, axis, dim, take_in, carry):
    whole = jax.tree.map(lambda part: lax.all_gather(part, axis, axis=dim, tiled=True), shard)
    return take_in(carry, whole, jnp.int32(0))


def over_all(shard, axis, dim, block):
    whole = lax.all_gather(shard, axis, axis=dim, tiled=True)
    return block(whole, jnp.int32(0))


def normalize(values, gain_vec):
    floats = values.astype(jnp.float32)
    scaled = floats * lax.rsqrt(jnp.mean(floats * floats, axis=-1, keepdims=True) + epsilon)
    return (scaled * gain_vec.astype(jnp.float32)).astype(jnp.bfloat16)


def half_step(local_part, gain_vec, gate_w, up_w, down_w):
    gathered = lax.all_gather(local_part, "tp", axis=2, tiled=True)
    seq_count, seq_length, full_width = gathered.shape
    normed = normalize(gathered.reshape(seq_count * seq_length, full_width), gain_vec)
    zero_init = jnp.zeros((normed.shape[0], gate_w.shape[1]), jnp.float32)

    def add_rows(running, block_rows, offset):
        columns = lax.dynamic_slice_in_dim(normed, offset, block_rows.shape[0], 1)
        return running + jnp.dot(columns, block_rows, preferred_element_type=jnp.float32)

    gate_sum = taken_in(gate_w, "fs", 0, add_rows, zero_init)
    up_sum = taken_in(up_w, "fs", 0, add_rows, zero_init)
    hidden = (jax.nn.silu(gate_sum) * up_sum).astype(jnp.bfloat16)

    def project(block_cols, offset):
        return jnp.dot(hidden, block_cols, preferred_element_type=jnp.float32)

    partial_value = over_all(down_w, "fs", 1, project)
    own_part = lax.psum_scatter(
        partial_value.astype(jnp.bfloat16), "tp", scatter_dimension=1, tiled=True
    ).astype(jnp.float32)
    return own_part.reshape(seq_count, seq_length, own_part.shape[1])


def trailing(grouped, windows, widest):
    seq_length = grouped.shape[1]
    running = jnp.zeros_like(grouped)
    for back_step in range(widest):
        moved = jnp.pad(grouped, ((0, 0), (back_step, 0), (0, 0), (0, 0)))[:, :seq_length]
        running = running + jnp.where(back_step < windows[None, None, :, None], moved, 0.0)
    positions = jnp.arange(seq_length, dtype=jnp.int32)
    counts = jnp.minimum(positions[:, None] + 1, windows[None, :]).astype(jnp.float32)
    return running / counts[None, :, :, None]


def pool_mix(local_part, mix_gain, pool_weight, pool_scale):
    floats = local_part.astype(jnp.float32)
    squares = lax.psum(jnp.sum(floats * floats, axis=-1).astype(jnp.bfloat16), "tp").astype(
        jnp.float32
    )
    normed = (
        floats * lax.rsqrt(squares[..., None] / D + epsilon) * mix_gain.astype(jnp.float32)
    ).astype(jnp.bfloat16)
    seq_count, seq_length, part_width = local_part.shape
    groups_here = pool_weight.shape[0]
    group_width = pool_weight.shape[1]
    grouped = normed.astype(jnp.float32).reshape(seq_count, seq_length, groups_here, group_width)
    group_ids = lax.axis_index("tp") * groups_here + jnp.arange(groups_here, dtype=jnp.int32)
    windows = 2 ** (group_ids + 1)
    pooled = trailing(grouped, windows, 2**GROUPS)
    diff = (pooled - grouped).astype(jnp.bfloat16)

    def mix_cols(block_cols, offset):
        return jnp.einsum("bsgc,gcd->bsgd", diff, block_cols, preferred_element_type=jnp.float32)

    mixed = over_all(pool_weight, "fs", 2, mix_cols)
    mixed = mixed.reshape(seq_count, seq_length, part_width)
    return (floats + mixed * pool_scale.astype(jnp.float32)).astype(jnp.bfloat16)


def local(
    tokens,
    pre_gain,
    first_gate,
    first_up,
    first_down,
    mix_gain,
    pool_weight,
    pool_scale,
    post_gain,
    second_gate,
    second_up,
    second_down,
):
    first_out = half_step(tokens, pre_gain, first_gate, first_up, first_down)
    after_first = (tokens.astype(jnp.float32) + 0.5 * first_out).astype(jnp.bfloat16)
    after_mix = pool_mix(after_first, mix_gain, pool_weight, pool_scale)
    second_out = half_step(after_mix, post_gain, second_gate, second_up, second_down)
    return (after_mix.astype(jnp.float32) + 0.5 * second_out).astype(jnp.bfloat16)


F32 = jnp.float32
BF16 = jnp.bfloat16


def layer_kernel(
    nz, tok_ref, pre_ref, mixg_ref, scale_ref, post_ref, pw_ref,
    g1_ref, u1_ref, d1_ref, g2_ref, u2_ref, d2_ref, out_ref,
    GU, DW, PW, T, N, ACC, H, PS, PR, S, R, SQ, TG, TL, tg_s,
    sw_s, sw_r, loc, zs, zr, ts, tr, cs, cr, os_, or_, ps_, pr_, qs, qr,
):
    r = lax.axis_index("rep")
    f = lax.axis_index("fs")
    t = lax.axis_index("tp")
    x = lax.rem(r, 2)
    y = lax.rem(f, 2)
    z = f // 2
    rx = r + 1 - 2 * x
    fy = f + 1 - 2 * y
    me = 2 * x + y
    other = 1 - t

    def dev(rr, ff, tt):
        return {"rep": rr, "fs": ff, "tp": tt}

    quad = (dev(rx, f, t), dev(r, fy, t), dev(rx, fy, t))
    quad_idx = (2 * (1 - x) + y, 2 * x + (1 - y), 2 * (1 - x) + (1 - y))
    mate = dev(r, f, other)
    above = dev(r, f + 2, t)
    below = dev(r, f - 2, t)
    has_above = z < nz - 1
    has_below = z > 0

    barrier = pltpu.get_barrier_semaphore()
    for peer in quad + (mate,):
        pl.semaphore_signal(barrier, inc=1, device_id=peer, device_id_type=pl.DeviceIdType.MESH)

    @pl.when(has_above)
    def _():
        pl.semaphore_signal(barrier, inc=1, device_id=above, device_id_type=pl.DeviceIdType.MESH)

    @pl.when(has_below)
    def _():
        pl.semaphore_signal(barrier, inc=1, device_id=below, device_id_type=pl.DeviceIdType.MESH)

    def remote(src, dst, ss, rs, to):
        return pltpu.make_async_remote_copy(
            src_ref=src, dst_ref=dst, send_sem=ss, recv_sem=rs,
            device_id=to, device_id_type=pl.DeviceIdType.MESH,
        )

    rows, half = tok_ref.shape
    depth = g1_ref.shape[0]
    main = (g1_ref.shape[1] // 512) * 128
    rest = g1_ref.shape[1] // 4 - main
    big = GU.shape[-1]
    cw = d1_ref.shape[1]
    weights = ((g1_ref, u1_ref, TL.at[0], d1_ref), (g2_ref, u2_ref, TL.at[1], d2_ref))

    def pieces(b, q):
        g, u, tl, d = weights[b]
        lanes = pl.ds(pl.multiple_of(q * main, 128), main)
        ends = pl.ds(pl.multiple_of(q * 2 * rest, 128), 2 * rest)
        deep = pl.ds(pl.multiple_of(y * depth, 128), depth)
        rows_main = pl.ds(pl.multiple_of(q * main, 128), main)
        rows_rest = pl.ds(pl.multiple_of(4 * main + q * rest, 16), rest)
        return (
            (g.at[:, lanes], GU.at[b, z, deep, 0:main]),
            (u.at[:, lanes], GU.at[b, z, deep, main:2 * main]),
            (tl.at[:, ends], GU.at[b, z, deep, 2 * main:big]),
            (d.at[rows_main, :], DW.at[b, z, y, 0:main, :]),
            (d.at[rows_rest, :], DW.at[b, z, y, main:main + rest, :]),
        )

    def tail_loads(b):
        return [
            pltpu.make_async_copy(weights[b][i].at[:, 4 * main:], TG.at[b, i], tg_s.at[b, i])
            for i in range(2)
        ]

    def tail_make(b):
        for c in tail_loads(b):
            c.wait()
        for q in range(4):
            cut = slice(q * rest, (q + 1) * rest)
            TL[b, :, q * 2 * rest:(q + 1) * 2 * rest] = jnp.concatenate(
                [TG[b, 0, :, cut], TG[b, 1, :, cut]], axis=1
            )

    def own_copies(b):
        found = [pltpu.make_async_copy(s, d, loc.at[b, i]) for i, (s, d) in enumerate(pieces(b, me))]
        if b == 0:
            found.append(pltpu.make_async_copy(pw_ref, PW.at[z, y], loc.at[b, 5]))
        return found

    def swaps(b):
        found = [
            remote(s, d, sw_s.at[b, i], sw_r.at[b, i], quad[1])
            for i, (s, d) in enumerate(pieces(b, quad_idx[1]))
        ]
        if b == 0:
            found.append(remote(pw_ref, PW.at[z, y], sw_s.at[b, 5], sw_r.at[b, 5], quad[1]))
        return found

    kinds = (GU, DW)

    def z_up(b, k, kind):
        p = jnp.maximum(z - k, 0)
        ref = PW.at[p] if kind == 2 else kinds[kind].at[b, p]
        return remote(ref, ref, zs.at[0, b, k, kind], zr.at[0, b, k, kind], above)

    def z_down(b, k, kind):
        p = jnp.minimum(z + k, nz - 1)
        ref = PW.at[p] if kind == 2 else kinds[kind].at[b, p]
        return remote(ref, ref, zs.at[1, b, k, kind], zr.at[1, b, k, kind], below)

    def can_up(k):
        return jnp.logical_and(has_above, z - k >= 0)

    def can_down(k):
        return jnp.logical_and(has_below, z + k <= nz - 1)

    def z_send(b, k, kind):
        @pl.when(can_up(k))
        def _():
            z_up(b, k, kind).start()

        @pl.when(can_down(k))
        def _():
            z_down(b, k, kind).start()

    def z_sent(b, k, kind):
        @pl.when(can_up(k))
        def _():
            z_up(b, k, kind).wait_send()

        @pl.when(can_down(k))
        def _():
            z_down(b, k, kind).wait_send()

    def z_take(b, k, kind):
        @pl.when(z - 1 - k >= 0)
        def _():
            z_up(b, k, kind).wait_recv()

        @pl.when(z + 1 + k <= nz - 1)
        def _():
            z_down(b, k, kind).wait_recv()

        if k + 1 < nz - 1:
            z_send(b, k + 1, kind)

    def tok_sends(b):
        mine = T.at[b, me, t]
        return [remote(mine, mine, ts.at[b, j], tr.at[b, j], quad[j]) for j in range(3)]

    def mate_own(b):
        mine = T.at[b, me, t]
        return remote(mine, mine, os_.at[b], or_.at[b], mate)

    def mate_pass(b, j):
        got = T.at[b, quad_idx[j], t]
        return remote(got, got, cs.at[b, j], cr.at[b, j], mate)

    def order(i):
        m = jnp.minimum(z, nz - 1 - z)
        near = z - (i + 1) // 2 if i % 2 else z + i // 2
        far = jnp.where(2 * z < nz - 1, i, nz - 1 - i)
        return jnp.where(i <= 2 * m, near, far)

    def norm_block(b, q, gain_ref):
        parts = [T[b, q, c].astype(F32) for c in range(2)]
        total = sum(jnp.sum(v * v, axis=-1, keepdims=True) for v in parts)
        inv = lax.rsqrt(total / (2 * half) + epsilon)
        step = N.shape[2]
        for c in range(2):
            done = (parts[c] * inv * gain_ref[0:1, c * half:(c + 1) * half]).astype(BF16)
            for i in range(half // step):
                N[c * (half // step) + i, pl.ds(pl.multiple_of(q * rows, 128), rows), :] = done[:, i * step:(i + 1) * step]

    def gate_up(b, i):
        p = order(i)

        @pl.loop(0, 4)
        def _(q):
            at = pl.ds(pl.multiple_of(q * rows, 128), rows)
            value = jnp.dot(N[p, at, :], GU[b, p], preferred_element_type=F32)
            if i == 0:
                ACC[at, :] = value
            else:
                ACC[at, :] += value

    turn = (quad_idx[2], quad_idx[0], quad_idx[1], me)
    turn_peer = (2, 0, 1)

    def rows_of(q):
        return pl.ds(pl.multiple_of(q * rows, 128), rows)

    def hidden_of(q):
        at = rows_of(q)
        gate = ACC[at, 0:main]
        up = ACC[at, main:2 * main]
        H[at, 0:main] = (jax.nn.silu(gate) * up).astype(BF16)
        last = ACC[at, 2 * main:big]
        H[at, main:main + rest] = (jax.nn.silu(last[:, :rest]) * last[:, rest:]).astype(BF16)

    def half_send(b, i):
        span = pl.ds(other * (nz // 2), nz // 2)
        q = turn[i]
        return remote(PS.at[b, q, span], PR.at[b, q], ps_.at[b, i], pr_.at[b, i], mate)

    def half_sends(b):
        return [half_send(b, i) for i in range(4)]

    def down(b, i):
        q = turn[i]
        for p in range(nz):
            wide = jnp.concatenate([DW[b, p, 0], DW[b, p, 1]], axis=1)
            PS[b, q, p] = jnp.dot(H[rows_of(q), :], wide, preferred_element_type=F32).astype(BF16)
        half_send(b, i).start()

    def quad_send(b, j):
        return remote(S.at[b, quad_idx[j]], R.at[b, j], qs.at[b, j], qr.at[b, j], quad[j])

    def quad_sends(b):
        return [quad_send(b, j) for j in range(3)]

    def sum_half(b, i):
        half_send(b, i).wait_recv()
        q = turn[i]
        for k in range(nz // 2):
            mine = PS[b, q, t * (nz // 2) + k].astype(F32)
            S[b, q, :, k * 2 * cw:(k + 1) * 2 * cw] = (mine + PR[b, q, k].astype(F32)).astype(BF16)
        if i < 3:
            quad_send(b, turn_peer[i]).start()

    def project(b, prepare):
        for i in range(4):
            prepare(turn[i])
            hidden_of(turn[i])
            down(b, i)
            if i:
                sum_half(b, i - 1)
        sum_half(b, 3)

    def chunk(b, i, q, fresh):
        p = order(i)
        value = jnp.dot(N[p, rows_of(q), :], GU[b, p], preferred_element_type=F32)
        if fresh:
            ACC[rows_of(q), :] = value
        else:
            ACC[rows_of(q), :] += value

    def collect(b):
        for send in quad_sends(b):
            send.wait_recv()
        total = S[b, me].astype(F32)
        for j in (2, 0, 1):
            total = total + R[b, j].astype(F32)
        return total

    for b in range(2):
        for c in tail_loads(b):
            c.start()
    T[0, me, t] = tok_ref[...]
    for b in range(2):
        tail_make(b)
    for c in own_copies(0):
        c.start()
    pl.semaphore_wait(
        barrier, 4 + jnp.minimum(z, 1) + jnp.minimum(nz - 1 - z, 1)
    )

    for c in swaps(0)[:5]:
        c.start()
    for j in (0, 2, 1):
        tok_sends(0)[j].start()
    mate_own(0).start()
    swaps(0)[5].start()
    for c in own_copies(1):
        c.start()
    for c in swaps(1):
        c.start()
    for i, c in enumerate(own_copies(0)):
        c.wait()
    for i in (0, 1, 2):
        swaps(0)[i].wait_recv()
    z_send(0, 0, 0)
    for i in (3, 4):
        swaps(0)[i].wait_recv()
    z_send(0, 0, 1)
    mate_own(0).wait_recv()
    norm_block(0, me, pre_ref)
    for j in (0, 2, 1):
        tok_sends(0)[j].wait_recv()
        mate_pass(0, j).start()
    for j in (0, 2, 1):
        mate_pass(0, j).wait_recv()
        norm_block(0, quad_idx[j], pre_ref)
    swaps(0)[5].wait_recv()
    gate_up(0, 0)
    for k in range(nz - 1):
        z_take(0, k, 0)
        gate_up(0, k + 1)
        z_take(0, k, 1)
        if k == 0:
            z_send(0, 0, 2)
        else:
            z_take(0, k - 1, 2)
        if k == max(nz - 3, 0):
            for c in own_copies(1):
                c.wait()
            for c in swaps(1):
                c.wait_recv()
            z_send(1, 0, 0)
            z_send(1, 0, 1)
    project(0, lambda q: None)
    z_take(0, nz - 2, 2)
    z_take(1, 0, 0)
    z_take(1, 0, 1)
    first = collect(0)
    after_first = (tok_ref[...].astype(F32) + 0.5 * first).astype(BF16).astype(F32)
    square = after_first * after_first
    SQ[0] = sum(square[:, i * 128:(i + 1) * 128] for i in range(half // 128))
    swap_sq = remote(SQ.at[0], SQ.at[1], os_.at[2], or_.at[2], mate)
    swap_sq.start()
    swap_sq.wait_recv()
    total = jnp.sum(SQ[0] + SQ[1], axis=-1, keepdims=True)
    h = (after_first * lax.rsqrt(total / (2 * half) + epsilon) * mixg_ref[0:1, :]).astype(BF16).astype(F32)
    position = lax.broadcasted_iota(jnp.int32, (rows, 128), 0)
    groups_here = pw_ref.shape[0]
    width = half // groups_here

    def shifted(v, by):
        place = lax.broadcasted_iota(jnp.int32, v.shape, 0)
        return jnp.where(place >= by, pltpu.roll(v, by, 0), 0.0)

    for g in range(groups_here):
        hg = h[:, g * width:(g + 1) * width]
        run = hg + shifted(hg, 1)
        window = 2
        found = run
        number = t * groups_here + g
        reached = jnp.int32(2)
        for level in range(1, GROUPS):
            run = run + shifted(run, window)
            window = window * 2
            found = jnp.where(number >= level, run, found)
            reached = jnp.where(number >= level, window, reached)
        counts = jnp.minimum(lax.broadcasted_iota(jnp.int32, (rows, width), 0) + 1, reached).astype(F32)
        diff = (found / counts - hg).astype(BF16)
        turned = jnp.concatenate([PW[i // 2, i % 2, g] for i in range(2 * nz)], axis=0)
        mixed = lax.dot_general(diff, turned, (((1,), (1,)), ((), ())), preferred_element_type=F32)
        at = slice(g * width, (g + 1) * width)
        T[1, me, t, :, at] = (after_first[:, at] + scale_ref[0:1, at] * mixed).astype(BF16)
    for j in (0, 2, 1):
        tok_sends(1)[j].start()
    mate_own(1).start()
    z_take(1, 1, 0)
    z_take(1, 1, 1)
    mate_own(1).wait_recv()
    norm_block(1, me, post_ref)
    for i in range(nz - 1):
        chunk(1, i, me, i == 0)
    for j in (0, 2, 1):
        tok_sends(1)[j].wait_recv()
        mate_pass(1, j).start()
    for j in (0, 2, 1):
        mate_pass(1, j).wait_recv()
        norm_block(1, quad_idx[j], post_ref)
        for i in range(nz - 1):
            chunk(1, i, quad_idx[j], i == 0)
    for k in range(2, nz - 1):
        z_take(1, k, 0)
        z_take(1, k, 1)
    project(1, lambda q: chunk(1, nz - 1, q, False))
    out_ref[...] = (T[1, me, t].astype(F32) + 0.5 * collect(1)).astype(BF16)

    for b in range(2):
        for c in swaps(b) + tok_sends(b) + [mate_own(b)] + [mate_pass(b, j) for j in range(3)]:
            c.wait_send()
        for c in half_sends(b) + quad_sends(b):
            c.wait_send()
        for k in range(nz - 1):
            for kind in range(3 if b == 0 else 2):
                z_sent(b, k, kind)
    swap_sq.wait_send()


def fused(
    fs, tokens, pre_gain, first_gate, first_up, first_down, mix_gain, pool_weight,
    pool_scale, post_gain, second_gate, second_up, second_down,
):
    nz = fs // 2
    _, rows, half = tokens.shape
    depth, hid = first_gate.shape
    cw = first_down.shape[1]
    main = (hid // 512) * 128
    rest = hid // 4 - main
    groups, width, out_cols = pool_weight.shape

    vmem = pl.BlockSpec(memory_space=pltpu.VMEM)
    anyw = pl.BlockSpec(memory_space=pl.ANY)
    dma = pltpu.SemaphoreType.DMA
    big = 2 * main + 2 * rest
    steps = nz - 1
    out = pl.pallas_call(
        functools.partial(layer_kernel, nz),
        out_shape=jax.ShapeDtypeStruct((rows, half), BF16),
        in_specs=[vmem] * 6 + [anyw] * 6,
        out_specs=vmem,
        scratch_shapes=[
            pltpu.VMEM((2, nz, 2 * depth, big), BF16),
            pltpu.VMEM((2, nz, 2, main + rest, cw), BF16),
            pltpu.VMEM((nz, 2, groups, out_cols, width), BF16),
            pltpu.VMEM((2, 4, 2, rows, half), BF16),
            pltpu.VMEM((nz, 4 * rows, 2 * depth), BF16),
            pltpu.VMEM((4 * rows, big), F32),
            pltpu.VMEM((4 * rows, main + rest), BF16),
            pltpu.VMEM((2, 4, nz, rows, 2 * cw), BF16),
            pltpu.VMEM((2, 4, nz // 2, rows, 2 * cw), BF16),
            pltpu.VMEM((2, 4, rows, half), BF16),
            pltpu.VMEM((2, 3, rows, half), BF16),
            pltpu.VMEM((2, rows, 128), F32),
            pltpu.VMEM((2, 2, depth, 4 * rest), BF16),
            pltpu.VMEM((2, depth, 8 * rest), BF16),
            dma((2, 2)),
            dma((2, 6)), dma((2, 6)), dma((2, 6)),
            dma((2, 2, steps, 3)), dma((2, 2, steps, 3)),
            dma((2, 3)), dma((2, 3)), dma((2, 3)), dma((2, 3)),
            dma((3,)), dma((3,)), dma((2, 4)), dma((2, 4)), dma((2, 3)), dma((2, 3)),
        ],
        compiler_params=pltpu.CompilerParams(
            collective_id=0, has_side_effects=True, vmem_limit_bytes=60 * 1024 * 1024
        ),
    )(
        tokens.reshape(rows, half), pre_gain.reshape(1, -1), mix_gain.reshape(1, -1),
        pool_scale.reshape(1, -1), post_gain.reshape(1, -1), jnp.swapaxes(pool_weight, 1, 2),
        first_gate, first_up, first_down, second_gate, second_up, second_down,
    )
    return out.reshape(tokens.shape)


def whole_tiles(mesh, args):
    reps, fs, tp = (mesh.shape[name] for name in ("rep", "fs", "tp"))
    depth = args[2].shape[0] // fs
    hid = args[2].shape[1] // tp
    return (
        tp == 2 and reps % 2 == 0 and fs % 8 == 0 and depth % 128 == 0
        and args[0].shape[0] == reps * fs and args[4].shape[1] // fs == depth
        and hid % 512 == 256 and args[6].shape[2] % (fs * 16) == 0
    )


def solution(mesh):
    placed = (
        P(("rep", "fs"), None, "tp"),
        P(),
        P("fs", "tp"),
        P("fs", "tp"),
        P("tp", "fs"),
        P("tp"),
        P("tp", None, "fs"),
        P("tp"),
        P(),
        P("fs", "tp"),
        P("fs", "tp"),
        P("tp", "fs"),
    )
    def layer(*args):
        body = functools.partial(fused, mesh.shape["fs"]) if whole_tiles(mesh, args) else local
        return jax.shard_map(
            body, mesh=mesh, in_specs=placed, out_specs=P(("rep", "fs"), None, "tp"), check_vma=False
        )(*args)

    return layer
```

```python
import functools

import jax
import jax.numpy as jnp
from jax import lax
from jax.experimental import pallas as pl
from jax.experimental.pallas import tpu as pltpu
from jax.sharding import PartitionSpec as P

D = 1024
GROUPS = 4


epsilon = 1e-06


def taken_in(shard, axis, dim, take_in, carry):
    whole = jax.tree.map(lambda part: lax.all_gather(part, axis, axis=dim, tiled=True), shard)
    return take_in(carry, whole, jnp.int32(0))


def over_all(shard, axis, dim, block):
    whole = lax.all_gather(shard, axis, axis=dim, tiled=True)
    return block(whole, jnp.int32(0))


def normalize(values, gain_vec):
    floats = values.astype(jnp.float32)
    scaled = floats * lax.rsqrt(jnp.mean(floats * floats, axis=-1, keepdims=True) + epsilon)
    return (scaled * gain_vec.astype(jnp.float32)).astype(jnp.bfloat16)


def half_step(local_part, gain_vec, gate_w, up_w, down_w):
    gathered = lax.all_gather(local_part, "tp", axis=2, tiled=True)
    seq_count, seq_length, full_width = gathered.shape
    normed = normalize(gathered.reshape(seq_count * seq_length, full_width), gain_vec)
    zero_init = jnp.zeros((normed.shape[0], gate_w.shape[1]), jnp.float32)

    def add_rows(running, block_rows, offset):
        columns = lax.dynamic_slice_in_dim(normed, offset, block_rows.shape[0], 1)
        return running + jnp.dot(columns, block_rows, preferred_element_type=jnp.float32)

    gate_sum = taken_in(gate_w, "fs", 0, add_rows, zero_init)
    up_sum = taken_in(up_w, "fs", 0, add_rows, zero_init)
    hidden = (jax.nn.silu(gate_sum) * up_sum).astype(jnp.bfloat16)

    def project(block_cols, offset):
        return jnp.dot(hidden, block_cols, preferred_element_type=jnp.float32)

    partial_value = over_all(down_w, "fs", 1, project)
    own_part = lax.psum_scatter(
        partial_value.astype(jnp.bfloat16), "tp", scatter_dimension=1, tiled=True
    ).astype(jnp.float32)
    return own_part.reshape(seq_count, seq_length, own_part.shape[1])


def trailing(grouped, windows, widest):
    seq_length = grouped.shape[1]
    running = jnp.zeros_like(grouped)
    for back_step in range(widest):
        moved = jnp.pad(grouped, ((0, 0), (back_step, 0), (0, 0), (0, 0)))[:, :seq_length]
        running = running + jnp.where(back_step < windows[None, None, :, None], moved, 0.0)
    positions = jnp.arange(seq_length, dtype=jnp.int32)
    counts = jnp.minimum(positions[:, None] + 1, windows[None, :]).astype(jnp.float32)
    return running / counts[None, :, :, None]


def pool_mix(local_part, mix_gain, pool_weight, pool_scale):
    floats = local_part.astype(jnp.float32)
    squares = lax.psum(jnp.sum(floats * floats, axis=-1).astype(jnp.bfloat16), "tp").astype(
        jnp.float32
    )
    normed = (
        floats * lax.rsqrt(squares[..., None] / D + epsilon) * mix_gain.astype(jnp.float32)
    ).astype(jnp.bfloat16)
    seq_count, seq_length, part_width = local_part.shape
    groups_here = pool_weight.shape[0]
    group_width = pool_weight.shape[1]
    grouped = normed.astype(jnp.float32).reshape(seq_count, seq_length, groups_here, group_width)
    group_ids = lax.axis_index("tp") * groups_here + jnp.arange(groups_here, dtype=jnp.int32)
    windows = 2 ** (group_ids + 1)
    pooled = trailing(grouped, windows, 2**GROUPS)
    diff = (pooled - grouped).astype(jnp.bfloat16)

    def mix_cols(block_cols, offset):
        return jnp.einsum("bsgc,gcd->bsgd", diff, block_cols, preferred_element_type=jnp.float32)

    mixed = over_all(pool_weight, "fs", 2, mix_cols)
    mixed = mixed.reshape(seq_count, seq_length, part_width)
    return (floats + mixed * pool_scale.astype(jnp.float32)).astype(jnp.bfloat16)


def local(
    tokens,
    pre_gain,
    first_gate,
    first_up,
    first_down,
    mix_gain,
    pool_weight,
    pool_scale,
    post_gain,
    second_gate,
    second_up,
    second_down,
):
    first_out = half_step(tokens, pre_gain, first_gate, first_up, first_down)
    after_first = (tokens.astype(jnp.float32) + 0.5 * first_out).astype(jnp.bfloat16)
    after_mix = pool_mix(after_first, mix_gain, pool_weight, pool_scale)
    second_out = half_step(after_mix, post_gain, second_gate, second_up, second_down)
    return (after_mix.astype(jnp.float32) + 0.5 * second_out).astype(jnp.bfloat16)


F32 = jnp.float32
BF16 = jnp.bfloat16


def layer_kernel(
    nz, tok_ref, pre_ref, mixg_ref, scale_ref, post_ref, pw_ref,
    g1_ref, u1_ref, d1_ref, g2_ref, u2_ref, d2_ref, out_ref,
    GU, DW, PW, T, N, ACC, H, PS, PR, S, R, SQ, TG, TL, tg_s,
    sw_s, sw_r, loc, zs, zr, ts, tr, cs, cr, os_, or_, ps_, pr_, qs, qr,
):
    r = lax.axis_index("rep")
    f = lax.axis_index("fs")
    t = lax.axis_index("tp")
    x = lax.rem(r, 2)
    y = lax.rem(f, 2)
    z = f // 2
    rx = r + 1 - 2 * x
    fy = f + 1 - 2 * y
    me = 2 * x + y
    other = 1 - t

    def dev(rr, ff, tt):
        return {"rep": rr, "fs": ff, "tp": tt}

    quad = (dev(rx, f, t), dev(r, fy, t), dev(rx, fy, t))
    quad_idx = (2 * (1 - x) + y, 2 * x + (1 - y), 2 * (1 - x) + (1 - y))
    mate = dev(r, f, other)
    above = dev(r, f + 2, t)
    below = dev(r, f - 2, t)
    has_above = z < nz - 1
    has_below = z > 0

    barrier = pltpu.get_barrier_semaphore()
    for peer in quad + (mate,):
        pl.semaphore_signal(barrier, inc=1, device_id=peer, device_id_type=pl.DeviceIdType.MESH)

    @pl.when(has_above)
    def _():
        pl.semaphore_signal(barrier, inc=1, device_id=above, device_id_type=pl.DeviceIdType.MESH)

    @pl.when(has_below)
    def _():
        pl.semaphore_signal(barrier, inc=1, device_id=below, device_id_type=pl.DeviceIdType.MESH)

    def remote(src, dst, ss, rs, to):
        return pltpu.make_async_remote_copy(
            src_ref=src, dst_ref=dst, send_sem=ss, recv_sem=rs,
            device_id=to, device_id_type=pl.DeviceIdType.MESH,
        )

    rows, half = tok_ref.shape
    depth = g1_ref.shape[0]
    main = (g1_ref.shape[1] // 512) * 128
    rest = g1_ref.shape[1] // 4 - main
    big = GU.shape[-1]
    cw = d1_ref.shape[1]
    weights = ((g1_ref, u1_ref, TL.at[0], d1_ref), (g2_ref, u2_ref, TL.at[1], d2_ref))

    def pieces(b, q):
        g, u, tl, d = weights[b]
        lanes = pl.ds(pl.multiple_of(q * main, 128), main)
        ends = pl.ds(pl.multiple_of(q * 2 * rest, 128), 2 * rest)
        deep = pl.ds(pl.multiple_of(y * depth, 128), depth)
        rows_main = pl.ds(pl.multiple_of(q * main, 128), main)
        rows_rest = pl.ds(pl.multiple_of(4 * main + q * rest, 16), rest)
        return (
            (g.at[:, lanes], GU.at[b, z, deep, 0:main]),
            (u.at[:, lanes], GU.at[b, z, deep, main:2 * main]),
            (tl.at[:, ends], GU.at[b, z, deep, 2 * main:big]),
            (d.at[rows_main, :], DW.at[b, z, y, 0:main, :]),
            (d.at[rows_rest, :], DW.at[b, z, y, main:main + rest, :]),
        )

    def tail_loads(b):
        return [
            pltpu.make_async_copy(weights[b][i].at[:, 4 * main:], TG.at[b, i], tg_s.at[b, i])
            for i in range(2)
        ]

    def tail_make(b):
        for c in tail_loads(b):
            c.wait()
        for q in range(4):
            cut = slice(q * rest, (q + 1) * rest)
            TL[b, :, q * 2 * rest:(q + 1) * 2 * rest] = jnp.concatenate(
                [TG[b, 0, :, cut], TG[b, 1, :, cut]], axis=1
            )

    def own_copies(b):
        found = [pltpu.make_async_copy(s, d, loc.at[b, i]) for i, (s, d) in enumerate(pieces(b, me))]
        if b == 0:
            found.append(pltpu.make_async_copy(pw_ref, PW.at[z, y], loc.at[b, 5]))
        return found

    def swaps(b):
        found = [
            remote(s, d, sw_s.at[b, i], sw_r.at[b, i], quad[1])
            for i, (s, d) in enumerate(pieces(b, quad_idx[1]))
        ]
        if b == 0:
            found.append(remote(pw_ref, PW.at[z, y], sw_s.at[b, 5], sw_r.at[b, 5], quad[1]))
        return found

    kinds = (GU, DW)

    def z_up(b, k, kind):
        p = jnp.maximum(z - k, 0)
        ref = PW.at[p] if kind == 2 else kinds[kind].at[b, p]
        return remote(ref, ref, zs.at[0, b, k, kind], zr.at[0, b, k, kind], above)

    def z_down(b, k, kind):
        p = jnp.minimum(z + k, nz - 1)
        ref = PW.at[p] if kind == 2 else kinds[kind].at[b, p]
        return remote(ref, ref, zs.at[1, b, k, kind], zr.at[1, b, k, kind], below)

    def can_up(k):
        return jnp.logical_and(has_above, z - k >= 0)

    def can_down(k):
        return jnp.logical_and(has_below, z + k <= nz - 1)

    def z_send(b, k, kind):
        @pl.when(can_up(k))
        def _():
            z_up(b, k, kind).start()

        @pl.when(can_down(k))
        def _():
            z_down(b, k, kind).start()

    def z_sent(b, k, kind):
        @pl.when(can_up(k))
        def _():
            z_up(b, k, kind).wait_send()

        @pl.when(can_down(k))
        def _():
            z_down(b, k, kind).wait_send()

    def z_pass(b, k, kind):
        @pl.when(jnp.logical_and(z - 1 - k >= 0, has_above))
        def _():
            z_up(b, k, kind).wait_recv()
            z_up(b, k + 1, kind).start()

        @pl.when(jnp.logical_and(z + 1 + k <= nz - 1, has_below))
        def _():
            z_down(b, k, kind).wait_recv()
            z_down(b, k + 1, kind).start()

    def z_end(b, k, kind):
        @pl.when(jnp.logical_and(z - 1 - k >= 0, z == nz - 1))
        def _():
            z_up(b, k, kind).wait_recv()

        @pl.when(jnp.logical_and(z + 1 + k <= nz - 1, z == 0))
        def _():
            z_down(b, k, kind).wait_recv()

    def z_take(b, k, kind):
        if k + 1 < nz - 1:
            z_pass(b, k, kind)
        z_end(b, k, kind)

    def tok_sends(b):
        mine = T.at[b, me, t]
        return [remote(mine, mine, ts.at[b, j], tr.at[b, j], quad[j]) for j in range(3)]

    def mate_own(b):
        mine = T.at[b, me, t]
        return remote(mine, mine, os_.at[b], or_.at[b], mate)

    def mate_pass(b, j):
        got = T.at[b, quad_idx[j], t]
        return remote(got, got, cs.at[b, j], cr.at[b, j], mate)

    def order(i):
        m = jnp.minimum(z, nz - 1 - z)
        near = z - (i + 1) // 2 if i % 2 else z + i // 2
        far = jnp.where(2 * z < nz - 1, i, nz - 1 - i)
        return jnp.where(i <= 2 * m, near, far)

    def norm_block(b, q, gain_ref):
        parts = [T[b, q, c].astype(F32) for c in range(2)]
        total = sum(jnp.sum(v * v, axis=-1, keepdims=True) for v in parts)
        inv = lax.rsqrt(total / (2 * half) + epsilon)
        step = N.shape[2]
        for c in range(2):
            done = (parts[c] * inv * gain_ref[0:1, c * half:(c + 1) * half]).astype(BF16)
            for i in range(half // step):
                N[c * (half // step) + i, pl.ds(pl.multiple_of(q * rows, 128), rows), :] = done[:, i * step:(i + 1) * step]

    def gate_up(b, i):
        p = order(i)

        @pl.loop(0, 4)
        def _(q):
            at = pl.ds(pl.multiple_of(q * rows, 128), rows)
            value = jnp.dot(N[p, at, :], GU[b, p], preferred_element_type=F32)
            if i == 0:
                ACC[at, :] = value
            else:
                ACC[at, :] += value

    turn = (quad_idx[2], quad_idx[0], quad_idx[1], me)
    turn_peer = (2, 0, 1)

    def rows_of(q):
        return pl.ds(pl.multiple_of(q * rows, 128), rows)

    def hidden_of(q):
        at = rows_of(q)
        gate = ACC[at, 0:main]
        up = ACC[at, main:2 * main]
        H[at, 0:main] = (jax.nn.silu(gate) * up).astype(BF16)
        last = ACC[at, 2 * main:big]
        H[at, main:main + rest] = (jax.nn.silu(last[:, :rest]) * last[:, rest:]).astype(BF16)

    def half_send(b, i):
        span = pl.ds(other * (nz // 2), nz // 2)
        q = turn[i]
        return remote(PS.at[b, q, span], PR.at[b, q], ps_.at[b, i], pr_.at[b, i], mate)

    def half_sends(b):
        return [half_send(b, i) for i in range(4)]

    def down(b, i):
        q = turn[i]
        for p in range(nz):
            wide = jnp.concatenate([DW[b, p, 0], DW[b, p, 1]], axis=1)
            PS[b, q, p] = jnp.dot(H[rows_of(q), :], wide, preferred_element_type=F32).astype(BF16)
        half_send(b, i).start()

    def quad_send(b, j):
        return remote(S.at[b, quad_idx[j]], R.at[b, j], qs.at[b, j], qr.at[b, j], quad[j])

    def quad_sends(b):
        return [quad_send(b, j) for j in range(3)]

    def sum_half(b, i):
        half_send(b, i).wait_recv()
        q = turn[i]
        for k in range(nz // 2):
            mine = PS[b, q, t * (nz // 2) + k].astype(F32)
            S[b, q, :, k * 2 * cw:(k + 1) * 2 * cw] = (mine + PR[b, q, k].astype(F32)).astype(BF16)
        if i < 3:
            quad_send(b, turn_peer[i]).start()

    def project(b, prepare):
        for i in range(4):
            prepare(turn[i])
            down(b, i)
            if i:
                sum_half(b, i - 1)
        sum_half(b, 3)

    def chunk(b, i, q, fresh):
        p = order(i)
        value = jnp.dot(N[p, rows_of(q), :], GU[b, p], preferred_element_type=F32)
        if fresh:
            ACC[rows_of(q), :] = value
        else:
            ACC[rows_of(q), :] += value

    def collect(b):
        for send in quad_sends(b):
            send.wait_recv()
        total = S[b, me].astype(F32)
        for j in (2, 0, 1):
            total = total + R[b, j].astype(F32)
        return total

    for b in range(2):
        for c in tail_loads(b):
            c.start()
    T[0, me, t] = tok_ref[...]
    for b in range(2):
        tail_make(b)
    for c in own_copies(0):
        c.start()
    pl.semaphore_wait(
        barrier, 4 + jnp.minimum(z, 1) + jnp.minimum(nz - 1 - z, 1)
    )

    for c in swaps(0)[:5]:
        c.start()
    for j in (0, 2, 1):
        tok_sends(0)[j].start()
    mate_own(0).start()
    swaps(0)[5].start()
    for c in own_copies(1):
        c.start()
    for c in swaps(1):
        c.start()
    for i, c in enumerate(own_copies(0)):
        c.wait()
    for i in (0, 1, 2):
        swaps(0)[i].wait_recv()
    z_send(0, 0, 0)
    for i in (3, 4):
        swaps(0)[i].wait_recv()
    z_send(0, 0, 1)
    mate_own(0).wait_recv()
    norm_block(0, me, pre_ref)
    for j in (0, 2, 1):
        tok_sends(0)[j].wait_recv()
        mate_pass(0, j).start()
    for j in (0, 2, 1):
        mate_pass(0, j).wait_recv()
        norm_block(0, quad_idx[j], pre_ref)
    swaps(0)[5].wait_recv()
    gate_up(0, 0)
    for k in range(nz - 1):
        z_take(0, k, 0)
        gate_up(0, k + 1)
        z_take(0, k, 1)
        if k == 0:
            z_send(0, 0, 2)
        else:
            z_take(0, k - 1, 2)
        if k == max(nz - 3, 0):
            for c in own_copies(1):
                c.wait()
            for c in swaps(1):
                c.wait_recv()
            z_send(1, 0, 0)
            z_send(1, 0, 1)
    project(0, hidden_of)
    z_take(0, nz - 2, 2)
    for k in range(nz - 2):
        z_pass(1, k, 0)
        z_pass(1, k, 1)
    first = collect(0)
    after_first = (tok_ref[...].astype(F32) + 0.5 * first).astype(BF16).astype(F32)
    square = after_first * after_first
    SQ[0] = sum(square[:, i * 128:(i + 1) * 128] for i in range(half // 128))
    swap_sq = remote(SQ.at[0], SQ.at[1], os_.at[2], or_.at[2], mate)
    swap_sq.start()
    swap_sq.wait_recv()
    total = jnp.sum(SQ[0] + SQ[1], axis=-1, keepdims=True)
    h = (after_first * lax.rsqrt(total / (2 * half) + epsilon) * mixg_ref[0:1, :]).astype(BF16).astype(F32)
    position = lax.broadcasted_iota(jnp.int32, (rows, 128), 0)
    groups_here = pw_ref.shape[0]
    width = half // groups_here

    def shifted(v, by):
        place = lax.broadcasted_iota(jnp.int32, v.shape, 0)
        return jnp.where(place >= by, pltpu.roll(v, by, 0), 0.0)

    for g in range(groups_here):
        hg = h[:, g * width:(g + 1) * width]
        run = hg + shifted(hg, 1)
        window = 2
        found = run
        number = t * groups_here + g
        reached = jnp.int32(2)
        for level in range(1, GROUPS):
            run = run + shifted(run, window)
            window = window * 2
            found = jnp.where(number >= level, run, found)
            reached = jnp.where(number >= level, window, reached)
        counts = jnp.minimum(lax.broadcasted_iota(jnp.int32, (rows, width), 0) + 1, reached).astype(F32)
        diff = (found / counts - hg).astype(BF16)
        turned = jnp.concatenate([PW[i // 2, i % 2, g] for i in range(2 * nz)], axis=0)
        mixed = lax.dot_general(diff, turned, (((1,), (1,)), ((), ())), preferred_element_type=F32)
        at = slice(g * width, (g + 1) * width)
        T[1, me, t, :, at] = (after_first[:, at] + scale_ref[0:1, at] * mixed).astype(BF16)
    for j in (0, 2, 1):
        tok_sends(1)[j].start()
    mate_own(1).start()
    for k in range(nz - 2):
        z_end(1, k, 0)
    mate_own(1).wait_recv()
    norm_block(1, me, post_ref)
    for i in range(nz - 1):
        chunk(1, i, me, i == 0)
    for j in (0, 2, 1):
        tok_sends(1)[j].wait_recv()
        mate_pass(1, j).start()
    for j in (0, 2, 1):
        mate_pass(1, j).wait_recv()
        norm_block(1, quad_idx[j], post_ref)
        for i in range(nz - 1):
            chunk(1, i, quad_idx[j], i == 0)
    z_end(1, nz - 2, 0)
    for q in turn:
        chunk(1, nz - 1, q, False)
        hidden_of(q)
    for k in range(nz - 1):
        z_end(1, k, 1)
    project(1, lambda q: None)
    out_ref[...] = (T[1, me, t].astype(F32) + 0.5 * collect(1)).astype(BF16)

    for b in range(2):
        for c in swaps(b) + tok_sends(b) + [mate_own(b)] + [mate_pass(b, j) for j in range(3)]:
            c.wait_send()
        for c in half_sends(b) + quad_sends(b):
            c.wait_send()
        for k in range(nz - 1):
            for kind in range(3 if b == 0 else 2):
                z_sent(b, k, kind)
    swap_sq.wait_send()


def fused(
    fs, tokens, pre_gain, first_gate, first_up, first_down, mix_gain, pool_weight,
    pool_scale, post_gain, second_gate, second_up, second_down,
):
    nz = fs // 2
    _, rows, half = tokens.shape
    depth, hid = first_gate.shape
    cw = first_down.shape[1]
    main = (hid // 512) * 128
    rest = hid // 4 - main
    groups, width, out_cols = pool_weight.shape

    vmem = pl.BlockSpec(memory_space=pltpu.VMEM)
    anyw = pl.BlockSpec(memory_space=pl.ANY)
    dma = pltpu.SemaphoreType.DMA
    big = 2 * main + 2 * rest
    steps = nz - 1
    out = pl.pallas_call(
        functools.partial(layer_kernel, nz),
        out_shape=jax.ShapeDtypeStruct((rows, half), BF16),
        in_specs=[vmem] * 6 + [anyw] * 6,
        out_specs=vmem,
        scratch_shapes=[
            pltpu.VMEM((2, nz, 2 * depth, big), BF16),
            pltpu.VMEM((2, nz, 2, main + rest, cw), BF16),
            pltpu.VMEM((nz, 2, groups, out_cols, width), BF16),
            pltpu.VMEM((2, 4, 2, rows, half), BF16),
            pltpu.VMEM((nz, 4 * rows, 2 * depth), BF16),
            pltpu.VMEM((4 * rows, big), F32),
            pltpu.VMEM((4 * rows, main + rest), BF16),
            pltpu.VMEM((2, 4, nz, rows, 2 * cw), BF16),
            pltpu.VMEM((2, 4, nz // 2, rows, 2 * cw), BF16),
            pltpu.VMEM((2, 4, rows, half), BF16),
            pltpu.VMEM((2, 3, rows, half), BF16),
            pltpu.VMEM((2, rows, 128), F32),
            pltpu.VMEM((2, 2, depth, 4 * rest), BF16),
            pltpu.VMEM((2, depth, 8 * rest), BF16),
            dma((2, 2)),
            dma((2, 6)), dma((2, 6)), dma((2, 6)),
            dma((2, 2, steps, 3)), dma((2, 2, steps, 3)),
            dma((2, 3)), dma((2, 3)), dma((2, 3)), dma((2, 3)),
            dma((3,)), dma((3,)), dma((2, 4)), dma((2, 4)), dma((2, 3)), dma((2, 3)),
        ],
        compiler_params=pltpu.CompilerParams(
            collective_id=0, has_side_effects=True, vmem_limit_bytes=60 * 1024 * 1024
        ),
    )(
        tokens.reshape(rows, half), pre_gain.reshape(1, -1), mix_gain.reshape(1, -1),
        pool_scale.reshape(1, -1), post_gain.reshape(1, -1), jnp.swapaxes(pool_weight, 1, 2),
        first_gate, first_up, first_down, second_gate, second_up, second_down,
    )
    return out.reshape(tokens.shape)


def whole_tiles(mesh, args):
    reps, fs, tp = (mesh.shape[name] for name in ("rep", "fs", "tp"))
    depth = args[2].shape[0] // fs
    hid = args[2].shape[1] // tp
    return (
        tp == 2 and reps % 2 == 0 and fs % 8 == 0 and depth % 128 == 0
        and args[0].shape[0] == reps * fs and args[4].shape[1] // fs == depth
        and hid % 512 == 256 and args[6].shape[2] % (fs * 16) == 0
    )


def solution(mesh):
    placed = (
        P(("rep", "fs"), None, "tp"),
        P(),
        P("fs", "tp"),
        P("fs", "tp"),
        P("tp", "fs"),
        P("tp"),
        P("tp", None, "fs"),
        P("tp"),
        P(),
        P("fs", "tp"),
        P("fs", "tp"),
        P("tp", "fs"),
    )
    def layer(*args):
        body = functools.partial(fused, mesh.shape["fs"]) if whole_tiles(mesh, args) else local
        return jax.shard_map(
            body, mesh=mesh, in_specs=placed, out_specs=P(("rep", "fs"), None, "tp"), check_vma=False
        )(*args)

    return layer
```
